32 devices in a mesh: sp: 4 (over x, core), dp: 8 (over z, y).
Axes of the slice: x: 2, y: 2, z: 4, core: 2. Of those that a mesh axis runs over, the one named last changes fastest.
Arguments:
- query: bfloat16 [8, 512, 1024], P('dp', None, 'sp'), may hold values from -120 to 120
- keys: bfloat16 [8, 512, 1024], P('dp', None, 'sp'), may hold values from -6 to 6
- values: bfloat16 [8, 512, 1024], P('dp', None, 'sp'), may hold values from -6 to 6
- output: bfloat16 [8, 512, 1024], P('dp'), may hold values from -1 to 1
- cum: float32 [8, 16, 512], P('dp', 'sp'), as said below
- d_out: bfloat16 [8, 512, 2048], P('dp', 'sp'), may hold values from -6 to 6
- w_out: bfloat16 [1024, 2048], P('dp'), may hold values from -0.125 to 0.125
Outputs:
- d_query: bfloat16 [8, 512, 1024], P('dp', 'sp')
- d_key: bfloat16 [8, 512, 1024], P('dp', 'sp')
- d_value: bfloat16 [8, 512, 1024], P('dp', 'sp')
- d_cum: float32 [8, 16, 512], P('dp', 'sp')
- d_w_out: float32 [1024, 2048], P('dp', 'sp')
The draws below stay inside these ranges and needn't reach their ends.
Inputs may be any that keep to these rules, and one draw needn't show every extreme that they name: cum never rises along positions.
All inputs are finite; a program needn't handle non-finite values.
Results may differ from the reference program's by a relative error of at most 0.008.
Values may be sent and summed in bfloat16 or wider, within the bound.
A program may use at most 64 MiB of HBM per device.

```python
import jax
import jax.numpy as jnp
from jax import lax

D = 2048
HEAD_TOTAL = 16
HEAD = 64
TOK_DEV = 128
ATTN = 1024
SEQUENCE_LENGTH = 512
SEQUENCE_COUNT = 8


def shared_keys(key):
    return jnp.clip(jax.random.normal(jax.random.fold_in(key, 11), (SEQUENCE_COUNT, SEQUENCE_LENGTH, ATTN), jnp.float32), -6.0, 6.0)


def draw_keys(key, part):
    return shared_keys(key).astype(jnp.bfloat16)


def draw_query(key, part):
    base_query = jnp.clip(jax.random.normal(jax.random.fold_in(key, 12), (SEQUENCE_COUNT, SEQUENCE_LENGTH, ATTN), jnp.float32), -6.0, 6.0)
    return base_query.astype(jnp.bfloat16)


def draw_cum(key, part):
    shape = (SEQUENCE_COUNT, HEAD_TOTAL, SEQUENCE_LENGTH)
    slow_share = 0.5
    slow_heads = jax.random.uniform(jax.random.fold_in(key, 21), (SEQUENCE_COUNT, HEAD_TOTAL, 1)) < slow_share
    fast_rate = jnp.exp(jax.random.uniform(jax.random.fold_in(key, 22), (SEQUENCE_COUNT, HEAD_TOTAL, 1), jnp.float32, jnp.log(1.0 / 60.0), jnp.log(1.0 / 25.0)))
    slow_rate = 0.7 / SEQUENCE_LENGTH * jnp.exp(jax.random.uniform(jax.random.fold_in(key, 23), (SEQUENCE_COUNT, HEAD_TOTAL, 1), jnp.float32, -0.7, 0.7))
    blocks = SEQUENCE_LENGTH // TOK_DEV
    block_factor = jnp.exp(jax.random.uniform(jax.random.fold_in(key, 24), (SEQUENCE_COUNT, HEAD_TOTAL, blocks), jnp.float32, -0.7, 0.7))
    block_factor = jnp.repeat(block_factor, TOK_DEV, axis=2)
    roughness = jax.random.uniform(jax.random.fold_in(key, 25), shape, jnp.float32, 0.3, 1.7)
    decay_rates = jnp.where(slow_heads, slow_rate, fast_rate) * block_factor * roughness
    spike_positions = jax.random.randint(jax.random.fold_in(key, 26), (SEQUENCE_COUNT, HEAD_TOTAL, 3), 0, SEQUENCE_LENGTH)
    spike_length = jnp.log(1.0 - jax.random.uniform(jax.random.fold_in(key, 27), (SEQUENCE_COUNT, HEAD_TOTAL, 3), jnp.float32, 0.2, 0.5))
    locations = jnp.arange(SEQUENCE_LENGTH)
    spikes = jnp.sum(jnp.where(locations[None, None, None, :] == spike_positions[:, :, :, None], spike_length[:, :, :, None], 0.0), axis=2)
    return jnp.cumsum(spikes - decay_rates, axis=2)


def raised(result, key, source, target, shards_of, factor):
    owner, partner = [(jnp.arange(result.shape[dim]) // (result.shape[dim] // shards_of)).reshape([-1 if axis == dim else 1 for axis in range(result.ndim)]) for dim in (source, target)]
    chosen = jax.random.permutation(key, shards_of)[partner]
    strong = (owner == chosen) | (owner == (partner + shards_of // 2) % shards_of)
    return jnp.where(strong, factor * result, result)


def level_of(rng, dims, pieces, low, high):
    factor_of, own = 1.0, jax.random.fold_in(rng, 6)
    for axis_at, parts in pieces:
        steps = jnp.exp(jax.random.uniform(jax.random.fold_in(own, axis_at), (parts,), jnp.float32, low / len(pieces), high / len(pieces)))
        factor_of = factor_of * jnp.repeat(steps, dims[axis_at] // parts).reshape([-1 if axis == axis_at else 1 for axis in range(len(dims))])
    return factor_of


def gaussian(stream_key, shape, width, bound, cuts=(), kind=jnp.bfloat16):
    array = jax.random.normal(stream_key, shape, jnp.float32) * width
    if len(cuts) > 0:
        array = level_of(stream_key, shape, cuts, -0.22, 0.18) * array
    return jnp.clip(array, min=-bound, max=bound).astype(kind)


def heavy_noise(key, extent, spread, limit, pieces, heavy, kind=jnp.bfloat16):
    array = spread * jax.random.normal(key, extent, jnp.float32)
    if pieces:
        array = array * level_of(key, extent, pieces, -0.22, 0.18)
    return jnp.clip(raised(array, jax.random.fold_in(key, 3), *heavy), -limit, limit).astype(kind)


def setup_inputs(seed: int = 0) -> dict:
    seeds = jax.random.split(jax.random.key(seed), 8)
    query = draw_query(jax.random.fold_in(seeds[7], 71), 0)
    keys = draw_keys(jax.random.fold_in(seeds[7], 71), 0)
    values = gaussian(seeds[2], (SEQUENCE_COUNT, SEQUENCE_LENGTH, ATTN), 1.0, 6.0, ((0, 8), (2, 4)))
    output = heavy_noise(seeds[3], (SEQUENCE_COUNT, SEQUENCE_LENGTH, ATTN), 0.125, 1.0, ((0, 8),), (0, 2, 8, 2.0))
    cum = draw_cum(jax.random.fold_in(seeds[7], 71), 0)
    d_out = gaussian(seeds[5], (SEQUENCE_COUNT, SEQUENCE_LENGTH, D), 1.0, 6.0, ((0, 8), (1, 4)))
    w_out = gaussian(seeds[6], (ATTN, D), D ** -0.5, 0.125, ((0, 8),))
    return {"query": query, "keys": keys, "values": values, "output": output, "cum": cum, "d_out": d_out, "w_out": w_out}


def product(left, right, form):
    return jnp.einsum(form, left.astype(jnp.float32), right.astype(jnp.float32))


def head_grads(query, keys, values, output, cotangent, cum):
    head_count, length, head_width = query.shape
    span_rows = min(512, length)
    score_scale = head_width ** -0.5
    row_dots = jnp.sum(cotangent.astype(jnp.float32) * output.astype(jnp.float32), axis=2)
    positions = jnp.arange(length)

    def advance(totals, block_index):
        key_grad, value_grad, cum_grad = totals
        offset = (block_index * span_rows).astype(jnp.int32)
        query_blk = lax.dynamic_slice_in_dim(query, offset, span_rows, 1)
        cot_blk = lax.dynamic_slice_in_dim(cotangent, offset, span_rows, 1)
        cum_blk = lax.dynamic_slice_in_dim(cum, offset, span_rows, 1)
        dots_blk = lax.dynamic_slice_in_dim(row_dots, offset, span_rows, 1)
        scores = product(query_blk, keys, "hqe,hke->hqk") * score_scale
        scores = scores + cum_blk[:, :, None] - cum[:, None, :]
        query_pos = offset + jnp.arange(span_rows)
        causal = positions[None, :] <= query_pos[:, None]
        scores = jnp.where(causal[None], scores, -1e30)
        row_max = jnp.max(scores, axis=2, keepdims=True)
        weights = jnp.exp(scores - row_max)
        weights = weights / jnp.sum(weights, axis=2, keepdims=True)
        weights_b = weights.astype(jnp.bfloat16)
        d_prob = product(cot_blk, values, "hqe,hke->hqk")
        d_score = weights * (d_prob - dots_blk[:, :, None])
        score_b = d_score.astype(jnp.bfloat16)
        query_grad = (product(score_b, keys, "hqk,hke->hqe") * score_scale).astype(jnp.bfloat16)
        key_grad = key_grad + product(score_b, query_blk, "hqk,hqe->hke") * score_scale
        value_grad = value_grad + product(weights_b, cot_blk, "hqk,hqe->hke")
        cum_grad = cum_grad - jnp.sum(d_score, axis=1)
        own_part = lax.dynamic_slice_in_dim(cum_grad, offset, span_rows, 1) + jnp.sum(d_score, axis=2)
        cum_grad = lax.dynamic_update_slice_in_dim(cum_grad, own_part, offset, 1)
        return (key_grad, value_grad, cum_grad), query_grad

    start_state = (jnp.zeros(query.shape, jnp.float32), jnp.zeros(query.shape, jnp.float32),
                   jnp.zeros(cum.shape, jnp.float32))
    totals, query_blocks = lax.scan(advance, start_state, jnp.arange(length // span_rows))
    query_grad = jnp.transpose(query_blocks, (1, 0, 2, 3)).reshape(query.shape)
    return query_grad, totals[0].astype(jnp.bfloat16), totals[1].astype(jnp.bfloat16), totals[2]


def reference(query, keys, values, output, cum, d_out, w_out):
    def one_sequence(sequence):
        q_seq, k_seq, v_seq, o_seq, c_seq, g_seq = sequence
        d_attn = jnp.dot(g_seq, w_out.T, preferred_element_type=jnp.float32).astype(jnp.bfloat16)

        def heads_first(matrix):
            return jnp.transpose(matrix.reshape(SEQUENCE_LENGTH, HEAD_TOTAL, HEAD), (1, 0, 2))

        def tokens_first(matrix):
            return jnp.transpose(matrix, (1, 0, 2)).reshape(SEQUENCE_LENGTH, ATTN)

        grads = head_grads(heads_first(q_seq), heads_first(k_seq), heads_first(v_seq),
                           heads_first(o_seq), heads_first(d_attn), c_seq)
        return tokens_first(grads[0]), tokens_first(grads[1]), tokens_first(grads[2]), grads[3]

    d_query, d_key, d_value, d_cum = lax.map(one_sequence, (query, keys, values, output, cum, d_out))

    def accumulate(running, couple):
        return running + jnp.dot(couple[0].T, couple[1], preferred_element_type=jnp.float32), None

    d_w_out = lax.scan(accumulate, jnp.zeros((ATTN, D), jnp.float32), (output, d_out))[0]
    return d_query, d_key, d_value, d_cum, d_w_out
```

```python
import functools

import jax
import jax.numpy as jnp
from jax import lax
from jax.experimental import pallas as pl
from jax.experimental.pallas import tpu as pltpu
from jax.sharding import PartitionSpec as P


def head_grads(query, keys, values, output, cotangent, cum):
    head_count, length, head_width = query.shape
    span_rows = min(512, length)
    score_scale = head_width ** (-0.5)
    row_dots = jnp.sum(cotangent.astype(jnp.float32) * output.astype(jnp.float32), axis=2)
    positions = jnp.arange(length)

    def product(left, right, form):
        return jnp.einsum(form, left, right, preferred_element_type=jnp.float32)

    def advance(totals, block_index):
        key_grad, value_grad, cum_grad = totals
        offset = block_index * span_rows
        query_blk = lax.dynamic_slice_in_dim(query, offset, span_rows, 1)
        cot_blk = lax.dynamic_slice_in_dim(cotangent, offset, span_rows, 1)
        cum_blk = lax.dynamic_slice_in_dim(cum, offset, span_rows, 1)
        dots_blk = lax.dynamic_slice_in_dim(row_dots, offset, span_rows, 1)
        scores = product(query_blk, keys, "hqe,hke->hqk") * score_scale
        scores = scores + cum_blk[:, :, None] - cum[:, None, :]
        query_pos = offset + jnp.arange(span_rows)
        causal = positions[None, :] <= query_pos[:, None]
        scores = jnp.where(causal[None], scores, -1e30)
        row_max = jnp.max(scores, axis=2, keepdims=True)
        weights = jnp.exp(scores - row_max)
        weights = weights / jnp.sum(weights, axis=2, keepdims=True)
        weights_b = weights.astype(jnp.bfloat16)
        d_prob = product(cot_blk, values, "hqe,hke->hqk")
        d_score = weights * (d_prob - dots_blk[:, :, None])
        score_b = d_score.astype(jnp.bfloat16)
        query_grad = (product(score_b, keys, "hqk,hke->hqe") * score_scale).astype(jnp.bfloat16)
        key_grad = key_grad + product(score_b, query_blk, "hqk,hqe->hke") * score_scale
        value_grad = value_grad + product(weights_b, cot_blk, "hqk,hqe->hke")
        cum_grad = cum_grad - jnp.sum(d_score, axis=1)
        own_part = lax.dynamic_slice_in_dim(cum_grad, offset, span_rows, 1) + jnp.sum(
            d_score, axis=2
        )
        cum_grad = lax.dynamic_update_slice_in_dim(cum_grad, own_part, offset, 1)
        return ((key_grad, value_grad, cum_grad), query_grad)

    start_state = (
        jnp.zeros(query.shape, jnp.float32),
        jnp.zeros(query.shape, jnp.float32),
        jnp.zeros(cum.shape, jnp.float32),
    )
    totals, query_blocks = lax.scan(advance, start_state, jnp.arange(length // span_rows))
    query_grad = jnp.transpose(query_blocks, (1, 0, 2, 3)).reshape(query.shape)
    return (query_grad, totals[0].astype(jnp.bfloat16), totals[1].astype(jnp.bfloat16), totals[2])


def shards(query, keys, values, output, cum, d_out, w_out):
    local_rows = d_out[0]
    whole_output = output[0]
    d_attn = lax.dot_general(
        local_rows,
        lax.all_gather(w_out, "dp", axis=0, tiled=True),
        (((1,), (1,)), ((), ())),
        preferred_element_type=jnp.float32,
    ).astype(jnp.bfloat16)
    head_cot, column_part = (
        lax.all_to_all(d_attn[None], "sp", split_axis=2, concat_axis=1, tiled=True),
        lax.all_to_all(d_out, "sp", split_axis=2, concat_axis=1, tiled=True),
    )
    grad_weight = lax.psum_scatter(
        lax.dot_general(
            whole_output,
            column_part[0],
            (((0,), (0,)), ((), ())),
            preferred_element_type=jnp.float32,
        ),
        "dp",
        scatter_dimension=0,
        tiled=True,
    )
    head_cols = query.shape[2]
    head_count = cum.shape[1]
    head_width = head_cols // head_count
    seq_length = query.shape[1]
    own_output = lax.dynamic_slice_in_dim(
        whole_output, lax.axis_index("sp") * head_cols, head_cols, 1
    )

    def heads_first(matrix):
        return jnp.transpose(matrix.reshape(seq_length, head_count, head_width), (1, 0, 2))

    def tokens_first(matrix):
        return jnp.transpose(matrix, (1, 0, 2)).reshape(1, seq_length, head_cols)

    grads = head_grads(
        heads_first(query[0]),
        heads_first(keys[0]),
        heads_first(values[0]),
        heads_first(own_output),
        heads_first(head_cot[0]),
        cum[0],
    )
    query_grad, key_grad, value_grad = (
        lax.all_to_all(tokens_first(grads[0]), "sp", split_axis=1, concat_axis=2, tiled=True),
        lax.all_to_all(tokens_first(grads[1]), "sp", split_axis=1, concat_axis=2, tiled=True),
        lax.all_to_all(tokens_first(grads[2]), "sp", split_axis=1, concat_axis=2, tiled=True),
    )
    return (query_grad, key_grad, value_grad, grads[3][None], grad_weight)


def plain_solution(mesh):
    placed = (
        P("dp", None, "sp"),
        P("dp", None, "sp"),
        P("dp", None, "sp"),
        P("dp", None, None),
        P("dp", "sp", None),
        P("dp", "sp", None),
        P("dp", None),
    )
    return jax.shard_map(
        shards,
        mesh=mesh,
        in_specs=placed,
        out_specs=(
            P("dp", "sp", None),
            P("dp", "sp", None),
            P("dp", "sp", None),
            P("dp", "sp", None),
            P("dp", "sp"),
        ),
        check_vma=False,
    )


MESH = pl.DeviceIdType.MESH
PAIR = 2
LANES = 128


def nt(left, right):
    return lax.dot_general(
        left, right, (((1,), (1,)), ((), ())), preferred_element_type=jnp.float32
    )


def nn(left, right):
    return lax.dot_general(
        left, right, (((1,), (0,)), ((), ())), preferred_element_type=jnp.float32
    )


def kernel(
    n_sp, n_dp, n_heads, w_chunks,
    q_hbm, k_hbm, v_hbm, o_hbm, cum_hbm, do_hbm, w_hbm,
    dq_out, dk_out, dv_out, dcum_out, dw_out,
    q_ref, k_ref, v_ref, o_ref, cum_ref, dof, wbuf, prob, k_t, o_t,
    dw_own, y_send, y_recv, z_send, z_recv, dw_acc, stage, dcum_ref,
    in_sem, out_sem,
    x_ssem, x_rsem, c_ssem, c_rsem, f_ssem, f_rsem,
    wz_ssem, wz_rsem, wy_ssem, wy_rsem,
    ry_ssem, ry_rsem, rz_ssem, rz_rsem,
    g_ssem, g_rsem, g_lsem,
):
    sp, dp = lax.axis_index("sp"), lax.axis_index("dp")
    n_x, n_z = n_sp // PAIR, n_dp // PAIR
    x, core = sp // PAIR, sp % PAIR
    z, y = dp // PAIR, dp % PAIR
    length, head_cols = q_ref.shape
    head_width = head_cols // n_heads
    tokens, width = do_hbm.shape[1:]
    w_rows = w_hbm.shape[0]
    col_part = width // n_sp
    scale = head_width ** (-0.5)
    per_pair = LANES // head_width
    n_pairs = head_cols // LANES
    block = min(2 * LANES, length)
    n_blocks = length // block
    core_peer = x * PAIR + (1 - core)
    y_peer = z * PAIR + (1 - y)

    def token_rows(owner):
        return pl.ds(pl.multiple_of(owner * tokens, tokens), tokens)

    def col_at(part):
        return pl.ds(pl.multiple_of(part * col_part, LANES), col_part)

    def remote(src, dst, ssem, rsem, **where):
        return pltpu.make_async_remote_copy(
            src_ref=src, dst_ref=dst, send_sem=ssem, recv_sem=rsem,
            device_id=where, device_id_type=MESH,
        )

    own_w = pl.ds(pl.multiple_of(y * w_rows, w_rows), w_rows)
    loads = [
        pltpu.make_async_copy(do_hbm.at[0], dof.at[token_rows(sp)], in_sem.at[0]),
        pltpu.make_async_copy(q_hbm.at[0], q_ref, in_sem.at[2]),
        pltpu.make_async_copy(k_hbm.at[0], k_ref, in_sem.at[3]),
        pltpu.make_async_copy(cum_hbm.at[0], cum_ref, in_sem.at[4]),
        pltpu.make_async_copy(v_hbm.at[0], v_ref, in_sem.at[5]),
        pltpu.make_async_copy(o_hbm.at[0], o_ref, in_sem.at[6]),
    ]
    w_load = pltpu.make_async_copy(w_hbm, wbuf.at[own_w], in_sem.at[1])
    loads[0].start()

    @pl.when(z == sp)
    def _():
        w_load.start()

    for load in loads[1:]:
        load.start()

    barrier = pltpu.get_barrier_semaphore()
    for off in range(1, n_sp):
        pl.semaphore_signal(
            barrier, inc=1, device_id={"sp": (sp + off) % n_sp, "dp": dp}, device_id_type=MESH
        )
    for off in range(1, n_z):
        pl.semaphore_signal(
            barrier, inc=1,
            device_id={"sp": sp, "dp": ((z + off) % n_z) * PAIR + y}, device_id_type=MESH,
        )
    pl.semaphore_signal(barrier, inc=1, device_id={"sp": sp, "dp": y_peer}, device_id_type=MESH)
    pl.semaphore_wait(barrier, n_sp + n_z - 1)

    def x_copy(off, i, owner_x, target_x):
        part = dof.at[token_rows(owner_x * PAIR + core), col_at((target_x * PAIR + i) % n_sp)]
        return remote(part, part, x_ssem.at[off - 1, i], x_rsem.at[off - 1, i],
                      sp=target_x * PAIR + core, dp=dp)

    def x_out(off, i):
        return x_copy(off, i, x, (x + off) % n_x)

    def x_in(off, i):
        return x_copy(off, i, (x + n_x - off) % n_x, x)

    def core_copy(owner):
        part = dof.at[token_rows(owner)]
        return remote(part, part, c_ssem, c_rsem, sp=core_peer, dp=dp)

    def forward_copy(off, i, owner_core):
        owner = ((x + n_x - off) % n_x) * PAIR + owner_core
        part = dof.at[token_rows(owner), col_at((x * PAIR + i) % n_sp)]
        return remote(part, part, f_ssem.at[off - 1, i], f_rsem.at[off - 1, i],
                      sp=core_peer, dp=dp)

    loads[0].wait()
    for i in range(n_sp):
        for off in range(1, n_x):
            x_out(off, i).start()
    core_copy(sp).start()

    def forward_step(i):
        for off in range(1, n_x):
            x_in(off, i).wait_recv()
            forward_copy(off, i, core).start()

    chunk_rows = w_rows // w_chunks

    def w_part(owner_y, c):
        start = pl.multiple_of(owner_y * w_rows + c * chunk_rows, chunk_rows)
        return wbuf.at[pl.ds(start, chunk_rows)]

    def wz_copy(way, c, target_z):
        return remote(w_part(y, c), w_part(y, c), wz_ssem.at[way, c], wz_rsem.at[c],
                      sp=sp, dp=target_z * PAIR + y)

    def wy_copy(owner_y, c):
        return remote(w_part(owner_y, c), w_part(owner_y, c), wy_ssem.at[c], wy_rsem.at[c],
                      sp=sp, dp=y_peer)

    sends_up = jnp.logical_and(z >= sp, z < n_z - 1)
    sends_down = jnp.logical_and(z <= sp, z > 0)

    def w_send(c):
        @pl.when(sends_up)
        def _():
            wz_copy(0, c, z + 1).start()

        @pl.when(sends_down)
        def _():
            wz_copy(1, c, z - 1).start()

        wy_copy(y, c).start()

    @pl.when(z == sp)
    def _():
        w_load.wait()
        for c in range(w_chunks):
            w_send(c)

    def w_step(c):
        @pl.when(z != sp)
        def _():
            wz_copy(0, c, z).wait_recv()
            w_send(c)

    lane = lax.broadcasted_iota(jnp.int32, (1, LANES), 1)

    def head_mask(h):
        return lane // head_width == h % per_pair

    def pair_cols(pair):
        return pl.ds(pair * LANES, LANES)

    for load in loads[1:4]:
        load.wait()
    cum = cum_ref[...]
    cum_cols = jnp.concatenate([cum] * (-(-8 // n_heads)), axis=0).T

    def masked_query(h):
        return jnp.where(head_mask(h), q_ref[:, pair_cols(h // per_pair)], 0)

    def probabilities(h):
        keys = k_ref[:, pair_cols(h // per_pair)]
        query = masked_query(h)
        for b in range(n_blocks):
            lo, end = b * block, (b + 1) * block
            scores = nt(keys[:end], query[lo:end]) * scale
            scores = scores + cum[h:h + 1, lo:end] - cum_cols[:end, h:h + 1]
            key_pos = lax.broadcasted_iota(jnp.int32, (end, block), 0)
            query_pos = lo + lax.broadcasted_iota(jnp.int32, (end, block), 1)
            scores = jnp.where(key_pos <= query_pos, scores, -1e30)
            weights = jnp.exp(scores - jnp.max(scores, axis=0, keepdims=True))
            weights = weights * (1.0 / jnp.sum(weights, axis=0, keepdims=True))
            prob[h, :end, lo:end] = weights

    steps = max(n_sp, w_chunks, n_heads)
    for i in range(steps):
        if i < n_heads:
            probabilities(i)
        if i == 0:
            k_t[...] = k_ref[...].T
        if i == 1:
            loads[4].wait()
            loads[5].wait()
            o_t[...] = o_ref[...].T
        if i < n_sp:
            forward_step(i)
        if i < w_chunks:
            w_step(i)

    core_copy(core_peer).wait_recv()
    for i in range(n_sp):
        for off in range(1, n_x):
            forward_copy(off, i, 1 - core).wait_recv()
    d_cols = dof[:, col_at(sp)]

    def z_at(k):
        return (z + k) % n_z

    def dw_rows(k, owner_y):
        return pl.ds(pl.multiple_of((z_at(k) * PAIR + owner_y) * w_rows, w_rows), w_rows)

    def ry_copy(k):
        return remote(y_send.at[k], y_recv.at[k], ry_ssem.at[k], ry_rsem.at[k], sp=sp, dp=y_peer)

    def rz_copy(k):
        return remote(z_send.at[k], z_recv.at[k], rz_ssem.at[k], rz_rsem.at[k],
                      sp=sp, dp=z_at(k) * PAIR + y)

    z_order = [k % n_z for k in range(1, n_z + 1)]
    for k in z_order:
        y_send[k] = nn(o_t[dw_rows(k, 1 - y), :], d_cols).astype(jnp.bfloat16)
        ry_copy(k).start()
    for k in z_order:
        dw_own[k] = nn(o_t[dw_rows(k, y), :], d_cols)

    def dw_step(k):
        ry_copy(k).wait_recv()
        total = dw_own[k] + y_recv[k].astype(jnp.float32)
        if k == 0:
            dw_acc[...] = total
        else:
            z_send[k] = total.astype(jnp.bfloat16)
            rz_copy(k).start()

    for c in range(w_chunks):
        wy_copy(1 - y, c).wait_recv()
    d_attn = nt(dof[...], wbuf[...]).astype(jnp.bfloat16)
    outs = (dq_out, dk_out, dv_out)

    def grad_copy(a, pair, off):
        target = (sp + off) % n_sp
        cols = pl.ds(pl.multiple_of(sp * head_cols + pair * LANES, LANES), LANES)
        return remote(stage.at[a, token_rows(target), pair_cols(pair)],
                      outs[a].at[0, :, cols],
                      g_ssem.at[a, pair, off - 1], g_rsem.at[a, pair, off - 1], sp=target, dp=dp)

    def grad_keep(a, pair):
        cols = pl.ds(pl.multiple_of(sp * head_cols + pair * LANES, LANES), LANES)
        return pltpu.make_async_copy(stage.at[a, token_rows(sp), pair_cols(pair)],
                                     outs[a].at[0, :, cols], g_lsem.at[a, pair])

    def add_rows(totals, part):
        for b in range(part.shape[0] // block):
            piece = part[b * block:(b + 1) * block]
            totals[b] = piece if totals[b] is None else totals[b] + piece

    def pair_gradients(pair):
        cot = d_attn[:, pair * LANES:(pair + 1) * LANES]
        own_out = o_ref[:, pl.ds(pl.multiple_of(sp * head_cols + pair * LANES, LANES), LANES)]
        values = v_ref[:, pair_cols(pair)]
        row = lax.broadcasted_iota(jnp.int32, (8, LANES), 0)
        picks = (lax.broadcasted_iota(jnp.int32, (8, LANES), 1) // head_width == row)
        dots = lax.dot_general(
            picks.astype(jnp.float32), cot.astype(jnp.float32) * own_out.astype(jnp.float32),
            (((1,), (1,)), ((), ())), precision=lax.Precision.HIGHEST,
            preferred_element_type=jnp.float32,
        )
        key_total, value_total, query_total = [None] * n_blocks, [None] * n_blocks, []
        for sub in range(per_pair):
            h = pair * per_pair + sub
            cot_h = jnp.where(head_mask(h), cot, 0)
            query_h = masked_query(h)
            keys_t = k_t[h * head_width:(h + 1) * head_width, :]
            query_parts, row_sums, col_sums = [], [], [None] * n_blocks
            for b in range(n_blocks):
                lo, end = b * block, (b + 1) * block
                weights = prob[h, :end, lo:end]
                d_prob = nt(values[:end], cot_h[lo:end])
                score_b = (weights * (d_prob - dots[sub:sub + 1, lo:end])).astype(jnp.bfloat16)
                add_rows(value_total, nn(weights.astype(jnp.bfloat16), cot_h[lo:end]))
                add_rows(key_total, nn(score_b, query_h[lo:end]))
                query_parts.append(nn(keys_t[:, :end], score_b))
                row_sums.append(nn(jnp.ones((8, end), jnp.bfloat16), score_b))
                col_sum = nt(jnp.ones((8, block), jnp.bfloat16), score_b)
                for j in range(b + 1):
                    piece = col_sum[:, j * block:(j + 1) * block]
                    col_sums[j] = piece if col_sums[j] is None else col_sums[j] + piece
            d_cum = jnp.concatenate(row_sums, axis=1) - jnp.concatenate(col_sums, axis=1)
            dcum_ref[h:h + 1, :] = d_cum[:1]
            query_total.append(jnp.concatenate(query_parts, axis=1))
        cols = pair_cols(pair)
        stage[0, :, cols] = (jnp.concatenate(query_total, axis=0).T * scale).astype(jnp.bfloat16)
        stage[1, :, cols] = (jnp.concatenate(key_total, axis=0) * scale).astype(jnp.bfloat16)
        stage[2, :, cols] = jnp.concatenate(value_total, axis=0).astype(jnp.bfloat16)
        for off in range(1, n_sp):
            for a in range(3):
                grad_copy(a, pair, off).start()
        for a in range(3):
            grad_keep(a, pair).start()

    todo = list(z_order)
    for pair in range(n_pairs):
        pair_gradients(pair)
        if todo:
            dw_step(todo.pop(0))
    while todo:
        dw_step(todo.pop(0))

    total = dw_acc[...]
    for k in range(1, n_z):
        rz_copy(k).wait_recv()
        total = total + z_recv[k].astype(jnp.float32)
    dw_acc[...] = total
    results = [
        pltpu.make_async_copy(dw_acc, dw_out, out_sem.at[0]),
        pltpu.make_async_copy(dcum_ref, dcum_out.at[0], out_sem.at[1]),
    ]
    for result in results:
        result.start()

    for i in range(n_sp):
        for off in range(1, n_x):
            x_out(off, i).wait_send()
            forward_copy(off, i, core).wait_send()
    core_copy(sp).wait_send()
    for c in range(w_chunks):
        wy_copy(y, c).wait_send()

        @pl.when(sends_up)
        def _():
            wz_copy(0, c, z + 1).wait_send()

        @pl.when(sends_down)
        def _():
            wz_copy(1, c, z - 1).wait_send()

    for k in range(n_z):
        ry_copy(k).wait_send()
        if k:
            rz_copy(k).wait_send()
    for pair in range(n_pairs):
        for a in range(3):
            for off in range(1, n_sp):
                grad_copy(a, pair, off).wait()
            grad_keep(a, pair).wait()
    for result in results:
        result.wait()


def fits(mesh, query, cum, d_out, w_out):
    n_sp, n_dp = mesh.shape["sp"], mesh.shape["dp"]
    head_cols, n_heads = query.shape[2] // n_sp, cum.shape[1] // n_sp
    length, width = d_out.shape[1], d_out.shape[2]
    w_rows = w_out.shape[0] // n_dp
    if head_cols % LANES or n_heads == 0 or 8 % n_heads:
        return False
    if LANES % (head_cols // n_heads) or length % (2 * LANES) or (width // n_sp) % LANES:
        return False
    if n_sp % PAIR or n_dp != PAIR * n_sp or head_cols != PAIR * w_rows or w_rows % 64:
        return False
    held = 4 * n_heads * length**2 + 2 * length * width + 8 * length * query.shape[2]
    return held < 32 * 2**20


def fused_shards(n_sp, n_dp, query, keys, values, output, cum, d_out, w_out):
    length, head_cols = query.shape[1:]
    attn = output.shape[2]
    n_heads = cum.shape[1]
    tokens, width = d_out.shape[1:]
    w_rows = w_out.shape[0]
    n_x, n_z, col_part = n_sp // PAIR, n_dp // PAIR, width // n_sp
    w_chunks = 4
    bf16, f32 = jnp.bfloat16, jnp.float32
    dma = pltpu.SemaphoreType.DMA
    n_pairs = head_cols // LANES
    anywhere = pl.BlockSpec(memory_space=pl.ANY)
    grad = jax.ShapeDtypeStruct((1, tokens, attn), bf16)
    return pl.pallas_call(
        functools.partial(kernel, n_sp, n_dp, n_heads, w_chunks),
        out_shape=(
            grad, grad, grad,
            jax.ShapeDtypeStruct(cum.shape, f32),
            jax.ShapeDtypeStruct((w_rows, col_part), f32),
        ),
        in_specs=[anywhere] * 7,
        out_specs=[anywhere] * 5,
        scratch_shapes=[
            pltpu.VMEM((length, head_cols), bf16),
            pltpu.VMEM((length, head_cols), bf16),
            pltpu.VMEM((length, head_cols), bf16),
            pltpu.VMEM((length, attn), bf16),
            pltpu.VMEM(cum.shape[1:], f32),
            pltpu.VMEM((length, width), bf16),
            pltpu.VMEM((PAIR * w_rows, width), bf16),
            pltpu.VMEM((n_heads, length, length), f32),
            pltpu.VMEM((head_cols, length), bf16),
            pltpu.VMEM((attn, length), bf16),
            pltpu.VMEM((n_z, w_rows, col_part), f32),
            pltpu.VMEM((n_z, w_rows, col_part), bf16),
            pltpu.VMEM((n_z, w_rows, col_part), bf16),
            pltpu.VMEM((n_z, w_rows, col_part), bf16),
            pltpu.VMEM((n_z, w_rows, col_part), bf16),
            pltpu.VMEM((w_rows, col_part), f32),
            pltpu.VMEM((3, length, head_cols), bf16),
            pltpu.VMEM(cum.shape[1:], f32),
            dma((7,)), dma((2,)),
            dma((n_x - 1, n_sp)), dma((n_x - 1, n_sp)), dma, dma,
            dma((n_x - 1, n_sp)), dma((n_x - 1, n_sp)),
            dma((2, w_chunks)), dma((w_chunks,)), dma((w_chunks,)), dma((w_chunks,)),
            dma((n_z,)), dma((n_z,)), dma((n_z,)), dma((n_z,)),
            dma((3, n_pairs, n_sp - 1)), dma((3, n_pairs, n_sp - 1)), dma((3, n_pairs)),
        ],
        compiler_params=pltpu.CompilerParams(
            collective_id=0, has_side_effects=True, vmem_limit_bytes=48 * 2**20
        ),
    )(query, keys, values, output, cum, d_out, w_out)


def solution(mesh):
    n_sp, n_dp = mesh.shape["sp"], mesh.shape["dp"]
    placed = (
        P("dp", None, "sp"), P("dp", None, "sp"), P("dp", None, "sp"), P("dp", None, None),
        P("dp", "sp", None), P("dp", "sp", None), P("dp", None),
    )
    results = (
        P("dp", "sp", None), P("dp", "sp", None), P("dp", "sp", None), P("dp", "sp", None),
        P("dp", "sp"),
    )

    def run(query, keys, values, output, cum, d_out, w_out):
        if fits(mesh, query, cum, d_out, w_out):
            body = functools.partial(fused_shards, n_sp, n_dp)
            step = jax.shard_map(
                body, mesh=mesh, in_specs=placed, out_specs=results, check_vma=False
            )
        else:
            step = plain_solution(mesh)
        return step(query, keys, values, output, cum, d_out, w_out)

    return run
```

```python
import functools

import jax
import jax.numpy as jnp
from jax import lax
from jax.experimental import pallas as pl
from jax.experimental.pallas import tpu as pltpu
from jax.sharding import PartitionSpec as P


def head_grads(query, keys, values, output, cotangent, cum):
    head_count, length, head_width = query.shape
    span_rows = min(512, length)
    score_scale = head_width ** (-0.5)
    row_dots = jnp.sum(cotangent.astype(jnp.float32) * output.astype(jnp.float32), axis=2)
    positions = jnp.arange(length)

    def product(left, right, form):
        return jnp.einsum(form, left, right, preferred_element_type=jnp.float32)

    def advance(totals, block_index):
        key_grad, value_grad, cum_grad = totals
        offset = block_index * span_rows
        query_blk = lax.dynamic_slice_in_dim(query, offset, span_rows, 1)
        cot_blk = lax.dynamic_slice_in_dim(cotangent, offset, span_rows, 1)
        cum_blk = lax.dynamic_slice_in_dim(cum, offset, span_rows, 1)
        dots_blk = lax.dynamic_slice_in_dim(row_dots, offset, span_rows, 1)
        scores = product(query_blk, keys, "hqe,hke->hqk") * score_scale
        scores = scores + cum_blk[:, :, None] - cum[:, None, :]
        query_pos = offset + jnp.arange(span_rows)
        causal = positions[None, :] <= query_pos[:, None]
        scores = jnp.where(causal[None], scores, -1e30)
        row_max = jnp.max(scores, axis=2, keepdims=True)
        weights = jnp.exp(scores - row_max)
        weights = weights / jnp.sum(weights, axis=2, keepdims=True)
        weights_b = weights.astype(jnp.bfloat16)
        d_prob = product(cot_blk, values, "hqe,hke->hqk")
        d_score = weights * (d_prob - dots_blk[:, :, None])
        score_b = d_score.astype(jnp.bfloat16)
        query_grad = (product(score_b, keys, "hqk,hke->hqe") * score_scale).astype(jnp.bfloat16)
        key_grad = key_grad + product(score_b, query_blk, "hqk,hqe->hke") * score_scale
        value_grad = value_grad + product(weights_b, cot_blk, "hqk,hqe->hke")
        cum_grad = cum_grad - jnp.sum(d_score, axis=1)
        own_part = lax.dynamic_slice_in_dim(cum_grad, offset, span_rows, 1) + jnp.sum(
            d_score, axis=2
        )
        cum_grad = lax.dynamic_update_slice_in_dim(cum_grad, own_part, offset, 1)
        return ((key_grad, value_grad, cum_grad), query_grad)

    start_state = (
        jnp.zeros(query.shape, jnp.float32),
        jnp.zeros(query.shape, jnp.float32),
        jnp.zeros(cum.shape, jnp.float32),
    )
    totals, query_blocks = lax.scan(advance, start_state, jnp.arange(length // span_rows))
    query_grad = jnp.transpose(query_blocks, (1, 0, 2, 3)).reshape(query.shape)
    return (query_grad, totals[0].astype(jnp.bfloat16), totals[1].astype(jnp.bfloat16), totals[2])


def shards(query, keys, values, output, cum, d_out, w_out):
    local_rows = d_out[0]
    whole_output = output[0]
    d_attn = lax.dot_general(
        local_rows,
        lax.all_gather(w_out, "dp", axis=0, tiled=True),
        (((1,), (1,)), ((), ())),
        preferred_element_type=jnp.float32,
    ).astype(jnp.bfloat16)
    head_cot, column_part = (
        lax.all_to_all(d_attn[None], "sp", split_axis=2, concat_axis=1, tiled=True),
        lax.all_to_all(d_out, "sp", split_axis=2, concat_axis=1, tiled=True),
    )
    grad_weight = lax.psum_scatter(
        lax.dot_general(
            whole_output,
            column_part[0],
            (((0,), (0,)), ((), ())),
            preferred_element_type=jnp.float32,
        ),
        "dp",
        scatter_dimension=0,
        tiled=True,
    )
    head_cols = query.shape[2]
    head_count = cum.shape[1]
    head_width = head_cols // head_count
    seq_length = query.shape[1]
    own_output = lax.dynamic_slice_in_dim(
        whole_output, lax.axis_index("sp") * head_cols, head_cols, 1
    )

    def heads_first(matrix):
        return jnp.transpose(matrix.reshape(seq_length, head_count, head_width), (1, 0, 2))

    def tokens_first(matrix):
        return jnp.transpose(matrix, (1, 0, 2)).reshape(1, seq_length, head_cols)

    grads = head_grads(
        heads_first(query[0]),
        heads_first(keys[0]),
        heads_first(values[0]),
        heads_first(own_output),
        heads_first(head_cot[0]),
        cum[0],
    )
    query_grad, key_grad, value_grad = (
        lax.all_to_all(tokens_first(grads[0]), "sp", split_axis=1, concat_axis=2, tiled=True),
        lax.all_to_all(tokens_first(grads[1]), "sp", split_axis=1, concat_axis=2, tiled=True),
        lax.all_to_all(tokens_first(grads[2]), "sp", split_axis=1, concat_axis=2, tiled=True),
    )
    return (query_grad, key_grad, value_grad, grads[3][None], grad_weight)


def plain_solution(mesh):
    placed = (
        P("dp", None, "sp"),
        P("dp", None, "sp"),
        P("dp", None, "sp"),
        P("dp", None, None),
        P("dp", "sp", None),
        P("dp", "sp", None),
        P("dp", None),
    )
    return jax.shard_map(
        shards,
        mesh=mesh,
        in_specs=placed,
        out_specs=(
            P("dp", "sp", None),
            P("dp", "sp", None),
            P("dp", "sp", None),
            P("dp", "sp", None),
            P("dp", "sp"),
        ),
        check_vma=False,
    )


MESH = pl.DeviceIdType.MESH
PAIR = 2
LANES = 128


def nt(left, right):
    return lax.dot_general(
        left, right, (((1,), (1,)), ((), ())), preferred_element_type=jnp.float32
    )


def nn(left, right):
    return lax.dot_general(
        left, right, (((1,), (0,)), ((), ())), preferred_element_type=jnp.float32
    )


def kernel(
    n_sp, n_dp, n_heads, w_chunks,
    q_hbm, k_hbm, v_hbm, o_hbm, cum_hbm, do_hbm, w_hbm,
    dq_out, dk_out, dv_out, dcum_out, dw_out,
    q_ref, k_ref, v_ref, o_ref, cum_ref, dof, wbuf, prob, k_t, o_t,
    dw_own, y_send, y_recv, z_send, z_recv, dw_acc, stage, dcum_ref,
    in_sem, out_sem,
    x_ssem, x_rsem, c_ssem, c_rsem, f_ssem, f_rsem,
    wz_ssem, wz_rsem, wy_ssem, wy_rsem,
    ry_ssem, ry_rsem, rz_ssem, rz_rsem,
    g_ssem, g_rsem, g_lsem,
):
    sp, dp = lax.axis_index("sp"), lax.axis_index("dp")
    n_x, n_z = n_sp // PAIR, n_dp // PAIR
    x, core = sp // PAIR, sp % PAIR
    z, y = dp // PAIR, dp % PAIR
    length, head_cols = q_ref.shape
    head_width = head_cols // n_heads
    tokens, width = do_hbm.shape[1:]
    w_rows = w_hbm.shape[0]
    col_part = width // n_sp
    scale = head_width ** (-0.5)
    per_pair = LANES // head_width
    n_pairs = head_cols // LANES
    block = min(2 * LANES, length)
    n_blocks = length // block
    core_peer = x * PAIR + (1 - core)
    y_peer = z * PAIR + (1 - y)

    def token_rows(owner):
        return pl.ds(pl.multiple_of(owner * tokens, tokens), tokens)

    def col_at(part):
        return pl.ds(pl.multiple_of(part * col_part, LANES), col_part)

    def remote(src, dst, ssem, rsem, **where):
        return pltpu.make_async_remote_copy(
            src_ref=src, dst_ref=dst, send_sem=ssem, recv_sem=rsem,
            device_id=where, device_id_type=MESH,
        )

    own_w = pl.ds(pl.multiple_of(y * w_rows, w_rows), w_rows)
    loads = [
        pltpu.make_async_copy(do_hbm.at[0], dof.at[token_rows(sp)], in_sem.at[0]),
        pltpu.make_async_copy(q_hbm.at[0], q_ref, in_sem.at[2]),
        pltpu.make_async_copy(k_hbm.at[0], k_ref, in_sem.at[3]),
        pltpu.make_async_copy(cum_hbm.at[0], cum_ref, in_sem.at[4]),
        pltpu.make_async_copy(v_hbm.at[0], v_ref, in_sem.at[5]),
        pltpu.make_async_copy(o_hbm.at[0], o_ref, in_sem.at[6]),
    ]
    w_load = pltpu.make_async_copy(w_hbm, wbuf.at[own_w], in_sem.at[1])
    loads[0].start()

    @pl.when(z == sp)
    def _():
        w_load.start()

    for load in loads[1:]:
        load.start()

    barrier = pltpu.get_barrier_semaphore()
    for off in range(1, n_sp):
        pl.semaphore_signal(
            barrier, inc=1, device_id={"sp": (sp + off) % n_sp, "dp": dp}, device_id_type=MESH
        )
    for off in range(1, n_z):
        pl.semaphore_signal(
            barrier, inc=1,
            device_id={"sp": sp, "dp": ((z + off) % n_z) * PAIR + y}, device_id_type=MESH,
        )
    pl.semaphore_signal(barrier, inc=1, device_id={"sp": sp, "dp": y_peer}, device_id_type=MESH)
    pl.semaphore_wait(barrier, n_sp + n_z - 1)

    def x_copy(off, i, owner_x, target_x):
        part = dof.at[token_rows(owner_x * PAIR + core), col_at((target_x * PAIR + i) % n_sp)]
        return remote(part, part, x_ssem.at[off - 1, i], x_rsem.at[off - 1, i],
                      sp=target_x * PAIR + core, dp=dp)

    def x_out(off, i):
        return x_copy(off, i, x, (x + off) % n_x)

    def x_in(off, i):
        return x_copy(off, i, (x + n_x - off) % n_x, x)

    def core_copy(owner):
        part = dof.at[token_rows(owner)]
        return remote(part, part, c_ssem, c_rsem, sp=core_peer, dp=dp)

    def forward_copy(off, i, owner_core):
        owner = ((x + n_x - off) % n_x) * PAIR + owner_core
        part = dof.at[token_rows(owner), col_at((x * PAIR + i) % n_sp)]
        return remote(part, part, f_ssem.at[off - 1, i], f_rsem.at[off - 1, i],
                      sp=core_peer, dp=dp)

    loads[0].wait()
    for i in range(n_sp):
        for off in range(1, n_x):
            x_out(off, i).start()
    core_copy(sp).start()

    def forward_step(i):
        for off in range(1, n_x):
            x_in(off, i).wait_recv()
            forward_copy(off, i, core).start()

    chunk_rows = w_rows // w_chunks

    def w_part(owner_y, c):
        start = pl.multiple_of(owner_y * w_rows + c * chunk_rows, chunk_rows)
        return wbuf.at[pl.ds(start, chunk_rows)]

    def wz_copy(way, c, target_z):
        return remote(w_part(y, c), w_part(y, c), wz_ssem.at[way, c], wz_rsem.at[c],
                      sp=sp, dp=target_z * PAIR + y)

    def wy_copy(owner_y, c):
        return remote(w_part(owner_y, c), w_part(owner_y, c), wy_ssem.at[c], wy_rsem.at[c],
                      sp=sp, dp=y_peer)

    sends_up = jnp.logical_and(z >= sp, z < n_z - 1)
    sends_down = jnp.logical_and(z <= sp, z > 0)

    def w_send(c):
        @pl.when(sends_up)
        def _():
            wz_copy(0, c, z + 1).start()

        @pl.when(sends_down)
        def _():
            wz_copy(1, c, z - 1).start()

        wy_copy(y, c).start()

    @pl.when(z == sp)
    def _():
        w_load.wait()
        for c in range(w_chunks):
            w_send(c)

    def w_step(c):
        @pl.when(z != sp)
        def _():
            wz_copy(0, c, z).wait_recv()
            w_send(c)

    lane = lax.broadcasted_iota(jnp.int32, (1, LANES), 1)

    def head_mask(h):
        return lane // head_width == h % per_pair

    def pair_cols(pair):
        return pl.ds(pair * LANES, LANES)

    for load in loads[1:4]:
        load.wait()
    cum = cum_ref[...]
    cum_cols = jnp.concatenate([cum] * (-(-8 // n_heads)), axis=0).T

    def masked_query(h):
        return jnp.where(head_mask(h), q_ref[:, pair_cols(h // per_pair)], 0)

    def probabilities(h):
        keys = k_ref[:, pair_cols(h // per_pair)]
        query = masked_query(h)
        for b in range(n_blocks):
            lo, end = b * block, (b + 1) * block
            scores = nt(keys[:end], query[lo:end]) * scale
            scores = scores + cum[h:h + 1, lo:end] - cum_cols[:end, h:h + 1]
            key_pos = lax.broadcasted_iota(jnp.int32, (end, block), 0)
            query_pos = lo + lax.broadcasted_iota(jnp.int32, (end, block), 1)
            scores = jnp.where(key_pos <= query_pos, scores, -1e30)
            weights = jnp.exp(scores - jnp.max(scores, axis=0, keepdims=True))
            weights = weights * (1.0 / jnp.sum(weights, axis=0, keepdims=True))
            prob[h, :end, lo:end] = weights

    steps = max(n_sp, w_chunks, n_heads)
    for i in range(steps):
        if i < n_heads:
            probabilities(i)
        if i == 0:
            k_t[...] = k_ref[...].T
        if i == 1:
            loads[4].wait()
            loads[5].wait()
            o_t[...] = o_ref[...].T
        if i < n_sp:
            forward_step(i)
        if i < w_chunks:
            w_step(i)

    core_copy(core_peer).wait_recv()
    for i in range(n_sp):
        for off in range(1, n_x):
            forward_copy(off, i, 1 - core).wait_recv()
    d_cols = dof[:, col_at(sp)]

    def z_at(k):
        return (z + k) % n_z

    def dw_rows(k, owner_y):
        return pl.ds(pl.multiple_of((z_at(k) * PAIR + owner_y) * w_rows, w_rows), w_rows)

    def ry_copy(k):
        return remote(y_send.at[k], y_recv.at[k], ry_ssem.at[k], ry_rsem.at[k], sp=sp, dp=y_peer)

    def rz_copy(k):
        return remote(z_send.at[k], z_recv.at[k], rz_ssem.at[k], rz_rsem.at[k],
                      sp=sp, dp=z_at(k) * PAIR + y)

    z_order = [k % n_z for k in range(1, n_z + 1)]
    for k in z_order:
        y_send[k] = nn(o_t[dw_rows(k, 1 - y), :], d_cols).astype(jnp.bfloat16)
        ry_copy(k).start()
    for k in z_order:
        dw_own[k] = nn(o_t[dw_rows(k, y), :], d_cols)

    def dw_step(k):
        ry_copy(k).wait_recv()
        total = dw_own[k] + y_recv[k].astype(jnp.float32)
        if k == 0:
            dw_acc[...] = total
        else:
            z_send[k] = total.astype(jnp.bfloat16)
            rz_copy(k).start()

    for c in range(w_chunks):
        wy_copy(1 - y, c).wait_recv()
    d_attn = nt(dof[...], wbuf[...]).astype(jnp.bfloat16)
    outs = (dq_out, dk_out, dv_out)

    def grad_copy(a, pair, off):
        target = (sp + off) % n_sp
        cols = pl.ds(pl.multiple_of(sp * head_cols + pair * LANES, LANES), LANES)
        return remote(stage.at[a, token_rows(target), pair_cols(pair)],
                      outs[a].at[0, :, cols],
                      g_ssem.at[a, pair, off - 1], g_rsem.at[a, pair, off - 1], sp=target, dp=dp)

    def grad_keep(a, pair):
        cols = pl.ds(pl.multiple_of(sp * head_cols + pair * LANES, LANES), LANES)
        return pltpu.make_async_copy(stage.at[a, token_rows(sp), pair_cols(pair)],
                                     outs[a].at[0, :, cols], g_lsem.at[a, pair])

    def add_rows(totals, part):
        for b in range(part.shape[0] // block):
            piece = part[b * block:(b + 1) * block]
            totals[b] = piece if totals[b] is None else totals[b] + piece

    def pair_gradients(pair):
        cot = d_attn[:, pair * LANES:(pair + 1) * LANES]
        own_out = o_ref[:, pl.ds(pl.multiple_of(sp * head_cols + pair * LANES, LANES), LANES)]
        values = v_ref[:, pair_cols(pair)]
        row = lax.broadcasted_iota(jnp.int32, (8, LANES), 0)
        picks = (lax.broadcasted_iota(jnp.int32, (8, LANES), 1) // head_width == row)
        dots = lax.dot_general(
            picks.astype(jnp.float32), cot.astype(jnp.float32) * own_out.astype(jnp.float32),
            (((1,), (1,)), ((), ())), precision=lax.Precision.HIGHEST,
            preferred_element_type=jnp.float32,
        )
        key_total, value_total, query_total = [None] * n_blocks, [None] * n_blocks, []
        for sub in range(per_pair):
            h = pair * per_pair + sub
            cot_h = jnp.where(head_mask(h), cot, 0)
            query_h = masked_query(h)
            keys_t = k_t[h * head_width:(h + 1) * head_width, :]
            query_parts, row_sums, col_sums = [], [], [None] * n_blocks
            for b in range(n_blocks):
                lo, end = b * block, (b + 1) * block
                weights = prob[h, :end, lo:end]
                d_prob = nt(values[:end], cot_h[lo:end])
                score_b = (weights * (d_prob - dots[sub:sub + 1, lo:end])).astype(jnp.bfloat16)
                add_rows(value_total, nn(weights.astype(jnp.bfloat16), cot_h[lo:end]))
                add_rows(key_total, nn(score_b, query_h[lo:end]))
                query_parts.append(nn(keys_t[:, :end], score_b))
                row_sums.append(nn(jnp.ones((8, end), jnp.bfloat16), score_b))
                col_sum = nt(jnp.ones((8, block), jnp.bfloat16), score_b)
                for j in range(b + 1):
                    piece = col_sum[:, j * block:(j + 1) * block]
                    col_sums[j] = piece if col_sums[j] is None else col_sums[j] + piece
            d_cum = jnp.concatenate(row_sums, axis=1) - jnp.concatenate(col_sums, axis=1)
            dcum_ref[h:h + 1, :] = d_cum[:1]
            query_total.append(jnp.concatenate(query_parts, axis=1))
        cols = pair_cols(pair)
        stage[0, :, cols] = (jnp.concatenate(query_total, axis=0).T * scale).astype(jnp.bfloat16)
        stage[1, :, cols] = (jnp.concatenate(key_total, axis=0) * scale).astype(jnp.bfloat16)
        stage[2, :, cols] = jnp.concatenate(value_total, axis=0).astype(jnp.bfloat16)
        for off in range(1, n_sp):
            for a in range(3):
                grad_copy(a, pair, off).start()
        for a in range(3):
            grad_keep(a, pair).start()

    todo = list(z_order)
    for pair in range(n_pairs):
        pair_gradients(pair)
        if todo:
            dw_step(todo.pop(0))
    while todo:
        dw_step(todo.pop(0))

    total = dw_acc[...]
    for k in range(1, n_z):
        rz_copy(k).wait_recv()
        total = total + z_recv[k].astype(jnp.float32)
    dw_acc[...] = total
    results = [
        pltpu.make_async_copy(dw_acc, dw_out, out_sem.at[0]),
        pltpu.make_async_copy(dcum_ref, dcum_out.at[0], out_sem.at[1]),
    ]
    for result in results:
        result.start()

    for i in range(n_sp):
        for off in range(1, n_x):
            x_out(off, i).wait_send()
            forward_copy(off, i, core).wait_send()
    core_copy(sp).wait_send()
    for c in range(w_chunks):
        wy_copy(y, c).wait_send()

        @pl.when(sends_up)
        def _():
            wz_copy(0, c, z + 1).wait_send()

        @pl.when(sends_down)
        def _():
            wz_copy(1, c, z - 1).wait_send()

    for k in range(n_z):
        ry_copy(k).wait_send()
        if k:
            rz_copy(k).wait_send()
    for pair in range(n_pairs):
        for a in range(3):
            for off in range(1, n_sp):
                grad_copy(a, pair, off).wait()
            grad_keep(a, pair).wait()
    for result in results:
        result.wait()


def hand_over(*refs):
    count = len(refs) // 2
    copies = [
        pltpu.make_async_copy(refs[i], refs[count + i], refs[-1].at[i]) for i in range(count)
    ]
    for copy in copies:
        copy.start()
    for copy in copies:
        copy.wait()


def fits(mesh, query, cum, d_out, w_out):
    n_sp, n_dp = mesh.shape["sp"], mesh.shape["dp"]
    head_cols, n_heads = query.shape[2] // n_sp, cum.shape[1] // n_sp
    length, width = d_out.shape[1], d_out.shape[2]
    w_rows = w_out.shape[0] // n_dp
    if head_cols % LANES or n_heads == 0 or 8 % n_heads:
        return False
    if LANES % (head_cols // n_heads) or length % (2 * LANES) or (width // n_sp) % LANES:
        return False
    if n_sp % PAIR or n_dp != PAIR * n_sp or head_cols != PAIR * w_rows or w_rows % 64:
        return False
    held = 4 * n_heads * length**2 + 2 * length * width + 8 * length * query.shape[2]
    return held < 32 * 2**20


def fused_shards(n_sp, n_dp, query, keys, values, output, cum, d_out, w_out):
    arrays = (query, keys, values, output, cum, d_out, w_out)
    length, head_cols = query.shape[1:]
    attn = output.shape[2]
    n_heads = cum.shape[1]
    tokens, width = d_out.shape[1:]
    w_rows = w_out.shape[0]
    n_x, n_z, col_part = n_sp // PAIR, n_dp // PAIR, width // n_sp
    w_chunks = 4
    bf16, f32 = jnp.bfloat16, jnp.float32
    dma = pltpu.SemaphoreType.DMA
    n_pairs = head_cols // LANES
    anywhere = pl.BlockSpec(memory_space=pl.ANY)
    from_hbm = pl.BlockSpec(memory_space=pltpu.HBM)
    grad = jax.ShapeDtypeStruct((1, tokens, attn), bf16)
    found = pl.pallas_call(
        functools.partial(kernel, n_sp, n_dp, n_heads, w_chunks),
        out_shape=(
            grad, grad, grad,
            jax.ShapeDtypeStruct(cum.shape, f32),
            jax.ShapeDtypeStruct((w_rows, col_part), f32),
        ),
        in_specs=[from_hbm] * 7,
        out_specs=[anywhere] * 5,
        scratch_shapes=[
            pltpu.VMEM((length, head_cols), bf16),
            pltpu.VMEM((length, head_cols), bf16),
            pltpu.VMEM((length, head_cols), bf16),
            pltpu.VMEM((length, attn), bf16),
            pltpu.VMEM(cum.shape[1:], f32),
            pltpu.VMEM((length, width), bf16),
            pltpu.VMEM((PAIR * w_rows, width), bf16),
            pltpu.VMEM((n_heads, length, length), f32),
            pltpu.VMEM((head_cols, length), bf16),
            pltpu.VMEM((attn, length), bf16),
            pltpu.VMEM((n_z, w_rows, col_part), f32),
            pltpu.VMEM((n_z, w_rows, col_part), bf16),
            pltpu.VMEM((n_z, w_rows, col_part), bf16),
            pltpu.VMEM((n_z, w_rows, col_part), bf16),
            pltpu.VMEM((n_z, w_rows, col_part), bf16),
            pltpu.VMEM((w_rows, col_part), f32),
            pltpu.VMEM((3, length, head_cols), bf16),
            pltpu.VMEM(cum.shape[1:], f32),
            dma((7,)), dma((2,)),
            dma((n_x - 1, n_sp)), dma((n_x - 1, n_sp)), dma, dma,
            dma((n_x - 1, n_sp)), dma((n_x - 1, n_sp)),
            dma((2, w_chunks)), dma((w_chunks,)), dma((w_chunks,)), dma((w_chunks,)),
            dma((n_z,)), dma((n_z,)), dma((n_z,)), dma((n_z,)),
            dma((3, n_pairs, n_sp - 1)), dma((3, n_pairs, n_sp - 1)), dma((3, n_pairs)),
        ],
        compiler_params=pltpu.CompilerParams(
            collective_id=0, has_side_effects=True, vmem_limit_bytes=48 * 2**20
        ),
    )(*[pltpu.with_memory_space_constraint(array, pltpu.HBM) for array in arrays])
    return pl.pallas_call(
        hand_over,
        out_shape=[jax.ShapeDtypeStruct(part.shape, part.dtype) for part in found],
        in_specs=[anywhere] * len(found),
        out_specs=[from_hbm] * len(found),
        scratch_shapes=[dma((len(found),))],
        compiler_params=pltpu.CompilerParams(vmem_limit_bytes=2**20),
    )(*found)


def solution(mesh):
    n_sp, n_dp = mesh.shape["sp"], mesh.shape["dp"]
    placed = (
        P("dp", None, "sp"), P("dp", None, "sp"), P("dp", None, "sp"), P("dp", None, None),
        P("dp", "sp", None), P("dp", "sp", None), P("dp", None),
    )
    results = (
        P("dp", "sp", None), P("dp", "sp", None), P("dp", "sp", None), P("dp", "sp", None),
        P("dp", "sp"),
    )

    def run(query, keys, values, output, cum, d_out, w_out):
        if fits(mesh, query, cum, d_out, w_out):
            body = functools.partial(fused_shards, n_sp, n_dp)
            step = jax.shard_map(
                body, mesh=mesh, in_specs=placed, out_specs=results, check_vma=False
            )
        else:
            step = plain_solution(mesh)
        return step(query, keys, values, output, cum, d_out, w_out)

    return run
```

```python
import functools

import jax
import jax.numpy as jnp
from jax import lax
from jax.experimental import pallas as pl
from jax.experimental.pallas import tpu as pltpu
from jax.sharding import PartitionSpec as P


def head_grads(query, keys, values, output, cotangent, cum):
    head_count, length, head_width = query.shape
    span_rows = min(512, length)
    score_scale = head_width ** (-0.5)
    row_dots = jnp.sum(cotangent.astype(jnp.float32) * output.astype(jnp.float32), axis=2)
    positions = jnp.arange(length)

    def product(left, right, form):
        return jnp.einsum(form, left, right, preferred_element_type=jnp.float32)

    def advance(totals, block_index):
        key_grad, value_grad, cum_grad = totals
        offset = block_index * span_rows
        query_blk = lax.dynamic_slice_in_dim(query, offset, span_rows, 1)
        cot_blk = lax.dynamic_slice_in_dim(cotangent, offset, span_rows, 1)
        cum_blk = lax.dynamic_slice_in_dim(cum, offset, span_rows, 1)
        dots_blk = lax.dynamic_slice_in_dim(row_dots, offset, span_rows, 1)
        scores = product(query_blk, keys, "hqe,hke->hqk") * score_scale
        scores = scores + cum_blk[:, :, None] - cum[:, None, :]
        query_pos = offset + jnp.arange(span_rows)
        causal = positions[None, :] <= query_pos[:, None]
        scores = jnp.where(causal[None], scores, -1e30)
        row_max = jnp.max(scores, axis=2, keepdims=True)
        weights = jnp.exp(scores - row_max)
        weights = weights / jnp.sum(weights, axis=2, keepdims=True)
        weights_b = weights.astype(jnp.bfloat16)
        d_prob = product(cot_blk, values, "hqe,hke->hqk")
        d_score = weights * (d_prob - dots_blk[:, :, None])
        score_b = d_score.astype(jnp.bfloat16)
        query_grad = (product(score_b, keys, "hqk,hke->hqe") * score_scale).astype(jnp.bfloat16)
        key_grad = key_grad + product(score_b, query_blk, "hqk,hqe->hke") * score_scale
        value_grad = value_grad + product(weights_b, cot_blk, "hqk,hqe->hke")
        cum_grad = cum_grad - jnp.sum(d_score, axis=1)
        own_part = lax.dynamic_slice_in_dim(cum_grad, offset, span_rows, 1) + jnp.sum(
            d_score, axis=2
        )
        cum_grad = lax.dynamic_update_slice_in_dim(cum_grad, own_part, offset, 1)
        return ((key_grad, value_grad, cum_grad), query_grad)

    start_state = (
        jnp.zeros(query.shape, jnp.float32),
        jnp.zeros(query.shape, jnp.float32),
        jnp.zeros(cum.shape, jnp.float32),
    )
    totals, query_blocks = lax.scan(advance, start_state, jnp.arange(length // span_rows))
    query_grad = jnp.transpose(query_blocks, (1, 0, 2, 3)).reshape(query.shape)
    return (query_grad, totals[0].astype(jnp.bfloat16), totals[1].astype(jnp.bfloat16), totals[2])


def shards(query, keys, values, output, cum, d_out, w_out):
    local_rows = d_out[0]
    whole_output = output[0]
    d_attn = lax.dot_general(
        local_rows,
        lax.all_gather(w_out, "dp", axis=0, tiled=True),
        (((1,), (1,)), ((), ())),
        preferred_element_type=jnp.float32,
    ).astype(jnp.bfloat16)
    head_cot, column_part = (
        lax.all_to_all(d_attn[None], "sp", split_axis=2, concat_axis=1, tiled=True),
        lax.all_to_all(d_out, "sp", split_axis=2, concat_axis=1, tiled=True),
    )
    grad_weight = lax.psum_scatter(
        lax.dot_general(
            whole_output,
            column_part[0],
            (((0,), (0,)), ((), ())),
            preferred_element_type=jnp.float32,
        ),
        "dp",
        scatter_dimension=0,
        tiled=True,
    )
    head_cols = query.shape[2]
    head_count = cum.shape[1]
    head_width = head_cols // head_count
    seq_length = query.shape[1]
    own_output = lax.dynamic_slice_in_dim(
        whole_output, lax.axis_index("sp") * head_cols, head_cols, 1
    )

    def heads_first(matrix):
        return jnp.transpose(matrix.reshape(seq_length, head_count, head_width), (1, 0, 2))

    def tokens_first(matrix):
        return jnp.transpose(matrix, (1, 0, 2)).reshape(1, seq_length, head_cols)

    grads = head_grads(
        heads_first(query[0]),
        heads_first(keys[0]),
        heads_first(values[0]),
        heads_first(own_output),
        heads_first(head_cot[0]),
        cum[0],
    )
    query_grad, key_grad, value_grad = (
        lax.all_to_all(tokens_first(grads[0]), "sp", split_axis=1, concat_axis=2, tiled=True),
        lax.all_to_all(tokens_first(grads[1]), "sp", split_axis=1, concat_axis=2, tiled=True),
        lax.all_to_all(tokens_first(grads[2]), "sp", split_axis=1, concat_axis=2, tiled=True),
    )
    return (query_grad, key_grad, value_grad, grads[3][None], grad_weight)


def plain_solution(mesh):
    placed = (
        P("dp", None, "sp"),
        P("dp", None, "sp"),
        P("dp", None, "sp"),
        P("dp", None, None),
        P("dp", "sp", None),
        P("dp", "sp", None),
        P("dp", None),
    )
    return jax.shard_map(
        shards,
        mesh=mesh,
        in_specs=placed,
        out_specs=(
            P("dp", "sp", None),
            P("dp", "sp", None),
            P("dp", "sp", None),
            P("dp", "sp", None),
            P("dp", "sp"),
        ),
        check_vma=False,
    )


MESH = pl.DeviceIdType.MESH
PAIR = 2
LANES = 128


def nt(left, right):
    return lax.dot_general(
        left, right, (((1,), (1,)), ((), ())), preferred_element_type=jnp.float32
    )


def nn(left, right):
    return lax.dot_general(
        left, right, (((1,), (0,)), ((), ())), preferred_element_type=jnp.float32
    )


def kernel(
    n_sp, n_dp, n_heads, w_chunks,
    q_hbm, k_hbm, v_hbm, o_hbm, cum_hbm, do_hbm, w_hbm,
    dq_out, dk_out, dv_out, dcum_out, dw_out,
    q_ref, k_ref, v_ref, o_ref, cum_ref, dof, wbuf, prob, k_t, o_t,
    dw_own, y_send, y_recv, z_send, z_recv, dw_acc, stage, dcum_ref,
    in_sem, out_sem,
    x_ssem, x_rsem, c_ssem, c_rsem, f_ssem, f_rsem,
    wz_ssem, wz_rsem, wy_ssem, wy_rsem,
    ry_ssem, ry_rsem, rz_ssem, rz_rsem,
    g_ssem, g_rsem, g_lsem,
):
    sp, dp = lax.axis_index("sp"), lax.axis_index("dp")
    n_x, n_z = n_sp // PAIR, n_dp // PAIR
    x, core = sp // PAIR, sp % PAIR
    z, y = dp // PAIR, dp % PAIR
    length, head_cols = q_ref.shape
    head_width = head_cols // n_heads
    tokens, width = do_hbm.shape[1:]
    w_rows = w_hbm.shape[0]
    col_part = width // n_sp
    scale = head_width ** (-0.5)
    per_pair = LANES // head_width
    n_pairs = head_cols // LANES
    block = min(2 * LANES, length)
    n_blocks = length // block
    core_peer = x * PAIR + (1 - core)
    y_peer = z * PAIR + (1 - y)

    def token_rows(owner):
        return pl.ds(pl.multiple_of(owner * tokens, tokens), tokens)

    def col_at(part):
        return pl.ds(pl.multiple_of(part * col_part, LANES), col_part)

    def remote(src, dst, ssem, rsem, **where):
        return pltpu.make_async_remote_copy(
            src_ref=src, dst_ref=dst, send_sem=ssem, recv_sem=rsem,
            device_id=where, device_id_type=MESH,
        )

    own_w = pl.ds(pl.multiple_of(y * w_rows, w_rows), w_rows)
    loads = [
        pltpu.make_async_copy(do_hbm.at[0], dof.at[token_rows(sp)], in_sem.at[0]),
        pltpu.make_async_copy(q_hbm.at[0], q_ref, in_sem.at[2]),
        pltpu.make_async_copy(k_hbm.at[0], k_ref, in_sem.at[3]),
        pltpu.make_async_copy(cum_hbm.at[0], cum_ref, in_sem.at[4]),
        pltpu.make_async_copy(v_hbm.at[0], v_ref, in_sem.at[5]),
        pltpu.make_async_copy(o_hbm.at[0], o_ref, in_sem.at[6]),
    ]
    w_load = pltpu.make_async_copy(w_hbm, wbuf.at[own_w], in_sem.at[1])
    loads[0].start()

    @pl.when(z == sp)
    def _():
        w_load.start()

    for load in loads[1:]:
        load.start()

    barrier = pltpu.get_barrier_semaphore()
    for off in range(1, n_sp):
        pl.semaphore_signal(
            barrier, inc=1, device_id={"sp": (sp + off) % n_sp, "dp": dp}, device_id_type=MESH
        )
    for off in range(1, n_z):
        pl.semaphore_signal(
            barrier, inc=1,
            device_id={"sp": sp, "dp": ((z + off) % n_z) * PAIR + y}, device_id_type=MESH,
        )
    pl.semaphore_signal(barrier, inc=1, device_id={"sp": sp, "dp": y_peer}, device_id_type=MESH)
    pl.semaphore_wait(barrier, n_sp + n_z - 1)

    def x_copy(off, i, owner_x, target_x):
        part = dof.at[token_rows(owner_x * PAIR + core), col_at((target_x * PAIR + i) % n_sp)]
        return remote(part, part, x_ssem.at[off - 1, i], x_rsem.at[off - 1, i],
                      sp=target_x * PAIR + core, dp=dp)

    def x_out(off, i):
        return x_copy(off, i, x, (x + off) % n_x)

    def x_in(off, i):
        return x_copy(off, i, (x + n_x - off) % n_x, x)

    def core_copy(owner):
        part = dof.at[token_rows(owner)]
        return remote(part, part, c_ssem, c_rsem, sp=core_peer, dp=dp)

    def forward_copy(off, i, owner_core):
        owner = ((x + n_x - off) % n_x) * PAIR + owner_core
        part = dof.at[token_rows(owner), col_at((x * PAIR + i) % n_sp)]
        return remote(part, part, f_ssem.at[off - 1, i], f_rsem.at[off - 1, i],
                      sp=core_peer, dp=dp)

    loads[0].wait()
    for i in range(n_sp):
        for off in range(1, n_x):
            x_out(off, i).start()
    core_copy(sp).start()

    def forward_step(i):
        for off in range(1, n_x):
            x_in(off, i).wait_recv()
            forward_copy(off, i, core).start()

    chunk_rows = w_rows // w_chunks

    def w_part(owner_y, c):
        start = pl.multiple_of(owner_y * w_rows + c * chunk_rows, chunk_rows)
        return wbuf.at[pl.ds(start, chunk_rows)]

    def wz_copy(way, c, target_z):
        return remote(w_part(y, c), w_part(y, c), wz_ssem.at[way, c], wz_rsem.at[c],
                      sp=sp, dp=target_z * PAIR + y)

    def wy_copy(owner_y, c):
        return remote(w_part(owner_y, c), w_part(owner_y, c), wy_ssem.at[c], wy_rsem.at[c],
                      sp=sp, dp=y_peer)

    sends_up = jnp.logical_and(z >= sp, z < n_z - 1)
    sends_down = jnp.logical_and(z <= sp, z > 0)

    def w_send(c):
        @pl.when(sends_up)
        def _():
            wz_copy(0, c, z + 1).start()

        @pl.when(sends_down)
        def _():
            wz_copy(1, c, z - 1).start()

        wy_copy(y, c).start()

    @pl.when(z == sp)
    def _():
        w_load.wait()
        for c in range(w_chunks):
            w_send(c)

    def w_step(c):
        @pl.when(z != sp)
        def _():
            wz_copy(0, c, z).wait_recv()
            w_send(c)

    lane = lax.broadcasted_iota(jnp.int32, (1, LANES), 1)

    def head_mask(sub):
        return lane // head_width == sub

    def pair_cols(pair):
        return pl.ds(pl.multiple_of(pair * LANES, LANES), LANES)

    for load in loads[1:4]:
        load.wait()
    cum = cum_ref[...]
    cum_cols = jnp.concatenate([cum] * (-(-8 // n_heads)), axis=0).T

    def masked_query(pair, sub):
        return jnp.where(head_mask(sub), q_ref[:, pair_cols(pair)], 0)

    def probabilities(h):
        keys = k_ref[:, pair_cols(h // per_pair)]
        query = masked_query(h // per_pair, h % per_pair)
        for b in range(n_blocks):
            lo, end = b * block, (b + 1) * block
            scores = nt(keys[:end], query[lo:end]) * scale
            scores = scores + cum[h:h + 1, lo:end] - cum_cols[:end, h:h + 1]
            key_pos = lax.broadcasted_iota(jnp.int32, (end, block), 0)
            query_pos = lo + lax.broadcasted_iota(jnp.int32, (end, block), 1)
            scores = jnp.where(key_pos <= query_pos, scores, -1e30)
            weights = jnp.exp(scores - jnp.max(scores, axis=0, keepdims=True))
            weights = weights * (1.0 / jnp.sum(weights, axis=0, keepdims=True))
            prob[h, :end, lo:end] = weights

    def key_transpose():
        k_t[...] = k_ref[...].T

    def output_transpose():
        loads[4].wait()
        loads[5].wait()
        o_t[...] = o_ref[...].T

    def z_at(k):
        bits = [(b, (z // b) % 2) for b in (2**i for i in range(n_z.bit_length() - 1))]
        return sum(b * (1 - bit if k & b else bit) for b, bit in bits)

    def dw_rows(k, owner_y):
        return pl.ds(pl.multiple_of((z_at(k) * PAIR + owner_y) * w_rows, w_rows), w_rows)

    def ry_copy(k):
        return remote(y_send.at[k], y_recv.at[k], ry_ssem.at[k], ry_rsem.at[k], sp=sp, dp=y_peer)

    def rz_copy(k):
        return remote(z_send.at[k], z_recv.at[k], rz_ssem.at[k], rz_rsem.at[k],
                      sp=sp, dp=z_at(k) * PAIR + y)

    half = n_z // 2
    z_order = list(range(half, n_z)) + list(range(half - 1, -1, -1))
    def columns_arrive(first, last):
        for i in range(first, last):
            for off in range(1, n_x):
                forward_copy(off, i, 1 - core).wait_recv()

    def columns_ready():
        core_copy(core_peer).wait_recv()
        columns_arrive(0, PAIR)

    def dw_away(n):
        k = z_order[n]
        product = nn(o_t[dw_rows(k, 1 - y), :], dof[:, col_at(sp)])
        y_send[k] = product.astype(jnp.bfloat16)

    def dw_keep(n):
        k = z_order[n]
        dw_own[k] = nn(o_t[dw_rows(k, y), :], dof[:, col_at(sp)])

    def dw_exchange(n):
        ry_copy(z_order[n]).start()

    def dw_step(n):
        k = z_order[n]
        ry_copy(k).wait_recv()
        total = dw_own[k] + y_recv[k].astype(jnp.float32)
        if k == 0:
            dw_acc[...] = total
        else:
            z_send[k] = total.astype(jnp.bfloat16)
            rz_copy(k).start()

    outs = (dq_out, dk_out, dv_out)

    def grad_cols(pair):
        return pl.ds(pl.multiple_of(sp * head_cols + pair * LANES, LANES), LANES)

    def pair_of(turn):
        return y if turn == 0 else 1 - y

    def grad_copy(a, turn, off):
        target = (sp + off) % n_sp
        pair = pair_of(turn)
        return remote(stage.at[a, token_rows(target), pair_cols(pair)],
                      outs[a].at[0, :, grad_cols(pair)],
                      g_ssem.at[a, turn, off - 1], g_rsem.at[a, turn, off - 1], sp=target, dp=dp)

    def grad_keep(a, turn):
        pair = pair_of(turn)
        return pltpu.make_async_copy(stage.at[a, token_rows(sp), pair_cols(pair)],
                                     outs[a].at[0, :, grad_cols(pair)], g_lsem.at[a, turn])

    def add_rows(totals, part):
        for b in range(part.shape[0] // block):
            piece = part[b * block:(b + 1) * block]
            totals[b] = piece if totals[b] is None else totals[b] + piece

    def pair_gradients(turn):
        pair = pair_of(turn)
        if turn:
            for c in range(w_chunks):
                wy_copy(1 - y, c).wait_recv()
        pair_w = wbuf[pl.ds(pl.multiple_of(pair * w_rows, w_rows), w_rows), :]
        cot = nt(dof[...], pair_w).astype(jnp.bfloat16)
        own_out = o_ref[:, grad_cols(pair)]
        values = v_ref[:, pair_cols(pair)]
        row = lax.broadcasted_iota(jnp.int32, (8, LANES), 0)
        picks = (lax.broadcasted_iota(jnp.int32, (8, LANES), 1) // head_width == row)
        dots = lax.dot_general(
            picks.astype(jnp.float32), cot.astype(jnp.float32) * own_out.astype(jnp.float32),
            (((1,), (1,)), ((), ())), precision=lax.Precision.HIGHEST,
            preferred_element_type=jnp.float32,
        )
        key_total, value_total, query_total = [None] * n_blocks, [None] * n_blocks, []
        for sub in range(per_pair):
            h = pair * per_pair + sub
            cot_h = jnp.where(head_mask(sub), cot, 0)
            query_h = masked_query(pair, sub)
            keys_t = k_t[pl.ds(pl.multiple_of(h * head_width, head_width), head_width), :]
            query_parts, row_sums, col_sums = [], [], [None] * n_blocks
            for b in range(n_blocks):
                lo, end = b * block, (b + 1) * block
                weights = prob[h, :end, lo:end]
                d_prob = nt(values[:end], cot_h[lo:end])
                score_b = (weights * (d_prob - dots[sub:sub + 1, lo:end])).astype(jnp.bfloat16)
                add_rows(value_total, nn(weights.astype(jnp.bfloat16), cot_h[lo:end]))
                add_rows(key_total, nn(score_b, query_h[lo:end]))
                query_parts.append(nn(keys_t[:, :end], score_b))
                row_sums.append(nn(jnp.ones((8, end), jnp.bfloat16), score_b))
                col_sum = nt(jnp.ones((8, block), jnp.bfloat16), score_b)
                for j in range(b + 1):
                    piece = col_sum[:, j * block:(j + 1) * block]
                    col_sums[j] = piece if col_sums[j] is None else col_sums[j] + piece
            d_cum = jnp.concatenate(row_sums, axis=1) - jnp.concatenate(col_sums, axis=1)
            dcum_ref[pl.ds(h, 1), :] = d_cum[:1]
            query_total.append(jnp.concatenate(query_parts, axis=1))
        cols = pair_cols(pair)
        stage[0, :, cols] = (jnp.concatenate(query_total, axis=0).T * scale).astype(jnp.bfloat16)
        stage[1, :, cols] = (jnp.concatenate(key_total, axis=0) * scale).astype(jnp.bfloat16)
        stage[2, :, cols] = jnp.concatenate(value_total, axis=0).astype(jnp.bfloat16)
        for off in range(1, n_sp):
            for a in range(3):
                grad_copy(a, turn, off).start()
        for a in range(3):
            grad_keep(a, turn).start()

    output_transpose()
    key_transpose()
    for h in range(n_heads):
        probabilities(h)
    sent = 0
    for i in range(n_sp):
        upto = min(w_chunks * (i + 1) // n_sp + 1, w_chunks)
        for c in range(sent, upto):
            w_step(c)
        sent = upto
        forward_step(i)
    columns_ready()
    for n in range(half):
        dw_away(n)
        dw_exchange(n)
    columns_arrive(PAIR, n_sp)
    pair_gradients(0)
    for n in range(half, n_z):
        dw_away(n)
        dw_exchange(n)
    for n in range(n_z):
        dw_keep(n)
    dw_step(0)
    pair_gradients(1)
    for n in range(1, n_z):
        dw_step(n)

    total = dw_acc[...]
    for k in range(1, n_z):
        rz_copy(k).wait_recv()
        total = total + z_recv[k].astype(jnp.float32)
    dw_acc[...] = total
    results = [
        pltpu.make_async_copy(dw_acc, dw_out, out_sem.at[0]),
        pltpu.make_async_copy(dcum_ref, dcum_out.at[0], out_sem.at[1]),
    ]
    for result in results:
        result.start()

    for i in range(n_sp):
        for off in range(1, n_x):
            x_out(off, i).wait_send()
            forward_copy(off, i, core).wait_send()
    core_copy(sp).wait_send()
    for c in range(w_chunks):
        wy_copy(y, c).wait_send()

        @pl.when(sends_up)
        def _():
            wz_copy(0, c, z + 1).wait_send()

        @pl.when(sends_down)
        def _():
            wz_copy(1, c, z - 1).wait_send()

    for k in range(n_z):
        ry_copy(k).wait_send()
        if k:
            rz_copy(k).wait_send()
    for turn in range(n_pairs):
        for a in range(3):
            for off in range(1, n_sp):
                grad_copy(a, turn, off).wait()
            grad_keep(a, turn).wait()
    for result in results:
        result.wait()


def hand_over(*refs):
    count = len(refs) // 2
    copies = [
        pltpu.make_async_copy(refs[i], refs[count + i], refs[-1].at[i]) for i in range(count)
    ]
    for copy in copies:
        copy.start()
    for copy in copies:
        copy.wait()


def fits(mesh, query, cum, d_out, w_out):
    n_sp, n_dp = mesh.shape["sp"], mesh.shape["dp"]
    head_cols, n_heads = query.shape[2] // n_sp, cum.shape[1] // n_sp
    length, width = d_out.shape[1], d_out.shape[2]
    w_rows = w_out.shape[0] // n_dp
    if head_cols % LANES or n_heads == 0 or 8 % n_heads:
        return False
    if LANES % (head_cols // n_heads) or length % (2 * LANES) or (width // n_sp) % LANES:
        return False
    if n_sp & (n_sp - 1) or n_sp < PAIR or n_dp != PAIR * n_sp or head_cols != PAIR * LANES or w_rows != LANES:
        return False
    held = 4 * n_heads * length**2 + 2 * length * width + 8 * length * query.shape[2]
    return held < 32 * 2**20


def fused_shards(n_sp, n_dp, query, keys, values, output, cum, d_out, w_out):
    arrays = (query, keys, values, output, cum, d_out, w_out)
    length, head_cols = query.shape[1:]
    attn = output.shape[2]
    n_heads = cum.shape[1]
    tokens, width = d_out.shape[1:]
    w_rows = w_out.shape[0]
    n_x, n_z, col_part = n_sp // PAIR, n_dp // PAIR, width // n_sp
    w_chunks = 8
    bf16, f32 = jnp.bfloat16, jnp.float32
    dma = pltpu.SemaphoreType.DMA
    n_pairs = head_cols // LANES
    anywhere = pl.BlockSpec(memory_space=pl.ANY)
    from_hbm = pl.BlockSpec(memory_space=pltpu.HBM)
    grad = jax.ShapeDtypeStruct((1, tokens, attn), bf16)
    found = pl.pallas_call(
        functools.partial(kernel, n_sp, n_dp, n_heads, w_chunks),
        out_shape=(
            grad, grad, grad,
            jax.ShapeDtypeStruct(cum.shape, f32),
            jax.ShapeDtypeStruct((w_rows, col_part), f32),
        ),
        in_specs=[from_hbm] * 7,
        out_specs=[anywhere] * 5,
        scratch_shapes=[
            pltpu.VMEM((length, head_cols), bf16),
            pltpu.VMEM((length, head_cols), bf16),
            pltpu.VMEM((length, head_cols), bf16),
            pltpu.VMEM((length, attn), bf16),
            pltpu.VMEM(cum.shape[1:], f32),
            pltpu.VMEM((length, width), bf16),
            pltpu.VMEM((PAIR * w_rows, width), bf16),
            pltpu.VMEM((n_heads, length, length), f32),
            pltpu.VMEM((head_cols, length), bf16),
            pltpu.VMEM((attn, length), bf16),
            pltpu.VMEM((n_z, w_rows, col_part), f32),
            pltpu.VMEM((n_z, w_rows, col_part), bf16),
            pltpu.VMEM((n_z, w_rows, col_part), bf16),
            pltpu.VMEM((n_z, w_rows, col_part), bf16),
            pltpu.VMEM((n_z, w_rows, col_part), bf16),
            pltpu.VMEM((w_rows, col_part), f32),
            pltpu.VMEM((3, length, head_cols), bf16),
            pltpu.VMEM(cum.shape[1:], f32),
            dma((7,)), dma((2,)),
            dma((n_x - 1, n_sp)), dma((n_x - 1, n_sp)), dma, dma,
            dma((n_x - 1, n_sp)), dma((n_x - 1, n_sp)),
            dma((2, w_chunks)), dma((w_chunks,)), dma((w_chunks,)), dma((w_chunks,)),
            dma((n_z,)), dma((n_z,)), dma((n_z,)), dma((n_z,)),
            dma((3, n_pairs, n_sp - 1)), dma((3, n_pairs, n_sp - 1)), dma((3, n_pairs)),
        ],
        compiler_params=pltpu.CompilerParams(
            collective_id=0, has_side_effects=True, vmem_limit_bytes=48 * 2**20
        ),
    )(*[pltpu.with_memory_space_constraint(array, pltpu.HBM) for array in arrays])
    return pl.pallas_call(
        hand_over,
        out_shape=[jax.ShapeDtypeStruct(part.shape, part.dtype) for part in found],
        in_specs=[anywhere] * len(found),
        out_specs=[from_hbm] * len(found),
        scratch_shapes=[dma((len(found),))],
        compiler_params=pltpu.CompilerParams(vmem_limit_bytes=2**20),
    )(*found)


def solution(mesh):
    n_sp, n_dp = mesh.shape["sp"], mesh.shape["dp"]
    placed = (
        P("dp", None, "sp"), P("dp", None, "sp"), P("dp", None, "sp"), P("dp", None, None),
        P("dp", "sp", None), P("dp", "sp", None), P("dp", None),
    )
    results = (
        P("dp", "sp", None), P("dp", "sp", None), P("dp", "sp", None), P("dp", "sp", None),
        P("dp", "sp"),
    )

    def run(query, keys, values, output, cum, d_out, w_out):
        if fits(mesh, query, cum, d_out, w_out):
            body = functools.partial(fused_shards, n_sp, n_dp)
            step = jax.shard_map(
                body, mesh=mesh, in_specs=placed, out_specs=results, check_vma=False
            )
        else:
            step = plain_solution(mesh)
        return step(query, keys, values, output, cum, d_out, w_out)

    return run
```
